32 devices in a mesh: ra: 4 (over z), cb: 4 (over y, x), dp: 2 (over core).
Axes of the slice: x: 2, y: 2, z: 4, core: 2. Of those that a mesh axis runs over, the one named last changes fastest.
Arguments:
- tokens: bfloat16 [3072, 4096], P('dp', 'ra'), may hold values from -20 to 20
- pre_gain: float32 [4096], P('ra'), may hold values from 0.1 to 1.9
- up_weight: bfloat16 [4096, 16384], P('ra', 'cb'), may hold values from -0.09375 to 0.09375
- up_bias: float32 [16384], P('cb'), may hold values from -4 to 4
- down_weight: bfloat16 [16384, 4096], P('cb', 'ra'), may hold values from -0.046875 to 0.046875
- post_gain: float32 [4096], P('ra'), may hold values from 0.1 to 1.9
Outputs:
- stream_out: bfloat16 [3072, 4096], P('dp', 'ra')
The draws below stay inside these ranges and needn't reach their ends.
All inputs are finite; a program needn't handle non-finite values.
Results may differ from the reference program's by a relative error of at most 0.0051.
Values may be sent and summed in bfloat16 or wider, within the bound.
A program may use at most 128 MiB of HBM per device.

```python
import jax
import jax.numpy as jnp
from jax import lax

D = 4096
FF = 16384
TOKENS = 3072


def draw_tokens(key, part):
    first, second, third = jax.random.split(key, 3)
    column = jnp.exp(jax.random.uniform(second, (D // 16,), jnp.float32, -1.2, 1.2))
    column = jnp.repeat(column, 16)
    values = jax.random.normal(first, (TOKENS, D), jnp.float32) * column
    return jnp.clip(values, -20.0, 20.0).astype(jnp.bfloat16)


def block_scale(rng, shape, cuts, low, largest):
    gain = 1.0
    for axis_at, shards_of in cuts:
        draws = jax.random.uniform(jax.random.fold_in(jax.random.fold_in(rng, 6), axis_at), (shards_of,), jnp.float32, low / len(cuts), largest / len(cuts))
        gain = gain * jnp.repeat(jnp.exp(draws), shape[axis_at] // shards_of).reshape((-1,) + (1,) * (len(shape) - 1 - axis_at))
    return gain


def bell_draw(own_key, shape, deviation, limit, shards=(), held_as=jnp.bfloat16):
    drawn = jax.random.normal(own_key, shape, jnp.float32) * deviation
    if len(shards) > 0:
        drawn = block_scale(own_key, shape, shards, -0.22, 0.18) * drawn
    return jnp.clip(drawn, min=-limit, max=limit).astype(held_as)


def setup_inputs(seed: int = 0) -> dict:
    seeds = jax.random.split(jax.random.key(seed), 7)
    return {
        "tokens": draw_tokens(jax.random.fold_in(seeds[6], 71), 0),
        "pre_gain": jnp.clip(1.0 + 0.18 * jax.random.normal(seeds[1], (D,), jnp.float32), 0.1, 1.9),
        "up_weight": bell_draw(seeds[2], (D, FF), D ** -0.5, 0.09375, ((0, 4), (1, 4))),
        "up_bias": bell_draw(seeds[3], (FF,), 1.0, 4.0, ((0, 4),), jnp.float32),
        "down_weight": bell_draw(seeds[4], (FF, D), FF ** -0.5, 0.046875, ((0, 4), (1, 4))),
        "post_gain": jnp.clip(1.0 + 0.18 * jax.random.normal(seeds[5], (D,), jnp.float32), 0.1, 1.9),
    }


epsilon = 1e-06
residual_weight = 0.5

def reference(tokens, pre_gain, up_weight, up_bias, down_weight, post_gain):
    stream = tokens.astype(jnp.float32)
    energy = lax.optimization_barrier(jnp.sum(stream * stream, axis=1))
    inverse = lax.rsqrt(energy / D + epsilon)
    scaled = (stream * pre_gain).astype(jnp.bfloat16)
    pre = jnp.dot(scaled, up_weight, preferred_element_type=jnp.float32) * inverse[:, None] + up_bias
    hidden = jnp.square(jax.nn.relu(pre)).astype(jnp.bfloat16)
    branch = jnp.dot(hidden, down_weight, preferred_element_type=jnp.float32)
    branch_energy = lax.optimization_barrier(jnp.sum(branch * branch, axis=1))
    normed = branch * lax.rsqrt(branch_energy / D + epsilon)[:, None] * post_gain
    return (residual_weight * stream + normed).astype(jnp.bfloat16)
```

```python
import functools

import jax
import jax.numpy as jnp
from jax import lax
from jax.experimental import pallas as pl
from jax.experimental.pallas import tpu as pltpu
from jax.sharding import PartitionSpec as P

epsilon = 1e-06
residual_weight = 0.5
MESH = pl.DeviceIdType.MESH
LANES = 128
MOST_FLAGS = 512


def pick(rows, ra, cb):
    small = 32
    while (2 * ra + 1) * (rows // small) > MOST_FLAGS and rows % (2 * small) == 0:
        small *= 2
    large = small
    while large // cb < 32 and rows % (2 * large) == 0:
        large *= 2
    return small, large


def kernel(n, m, g, big, tokens, mine, up, down, pre_gain, bias, post_gain, out,
           xs, uw, dw, rr, hg, ys, yo, yr, os, xq, acc, po, e, inv, be,
           load_sem, right_sem, left_sem, rs_sem, hg_sem, y_send, yr_sem, o_send, out_sem, out_local,
           e_send, e_sem, be_send, be_sem):
    rows, depth = xs.shape
    width = depth * n
    units = hg.shape[2]
    few = big // m
    count, blocks, per = rows // g, rows // big, big // g
    z, c = lax.axis_index("ra"), lax.axis_index("cb")
    first, last = z == 0, z == n - 1

    def at(j, size):
        return pl.ds(pl.multiple_of(j * size, size), size)

    def remote(src, dst, send, recv, **where):
        return pltpu.make_async_remote_copy(src, dst, send, recv, device_id=where, device_id_type=MESH)

    loads = [pltpu.make_async_copy(tokens, ys, load_sem.at[0])]
    loads += [pltpu.make_async_copy(up.at[:, pl.ds(s * units, units)], uw.at[s], load_sem.at[1 + s]) for s in range(n)]
    loads += [pltpu.make_async_copy(mine.at[:, c], xq, load_sem.at[1 + n])]
    loads += [pltpu.make_async_copy(down, dw, load_sem.at[2 + n])]
    for load in loads:
        load.start()

    barrier = pltpu.get_barrier_semaphore()
    for d in range(1, n):
        pl.semaphore_signal(barrier, inc=1, device_id={"ra": lax.rem(z + d, n)}, device_id_type=MESH)
    for d in range(1, m):
        pl.semaphore_signal(barrier, inc=1, device_id={"cb": lax.rem(c + d, m)}, device_id_type=MESH)
    pl.semaphore_wait(barrier, n + m - 2)

    loads[0].wait()

    @pl.loop(0, rows // LANES)
    def _(b):
        part = at(b, LANES)
        raw = ys[part, :].astype(jnp.float32)
        xs[part, :] = (raw * pre_gain[...]).astype(jnp.bfloat16)
        total = jnp.sum(raw * raw, axis=1, keepdims=True)
        e[z, :, part] = jnp.broadcast_to(total, (LANES, LANES)).T[:8, :]

    for load in loads[1:]:
        load.wait()
    for d in range(1, n):
        remote(e.at[z], e.at[z], e_send.at[d], e_sem.at[z], ra=lax.rem(z + d, n)).start()

    def dot(a, b):
        return jnp.dot(a, b, preferred_element_type=jnp.float32)

    def to_right(src, dst, flag):
        remote(src, dst, right_sem, flag, ra=jnp.minimum(z + 1, n - 1)).start()

    def to_left(src, dst, flag):
        remote(src, dst, left_sem, flag, ra=jnp.maximum(z - 1, 0)).start()

    def arrived(ref, flag):
        pltpu.make_async_copy(ref, ref, flag).wait()

    def step(i, _):
        @pl.when(i == n - 1)
        def _():
            for d in range(1, n):
                s = lax.rem(z + d, n)
                arrived(e.at[s], e_sem.at[s])

            @pl.loop(0, rows // LANES)
            def _(b):
                part = at(b, LANES)
                total = e[0, :, part]
                for s in range(1, n):
                    total = total + e[s, :, part]
                factor = lax.rsqrt(total / width + epsilon)
                inv[part, :] = jnp.broadcast_to(factor[:1, :], (LANES, LANES)).T

        j = i - n

        @pl.when(jnp.logical_and(j >= 0, j < count))
        def _():
            here = at(j, g)
            po[...] = dot(xs[here, :], uw[z])

            @pl.when(jnp.logical_not(first))
            def _():
                arrived(rr.at[z, here], rs_sem.at[z, j])
                po[...] += rr[z, here, :].astype(jnp.float32)

            @pl.when(jnp.logical_not(last))
            def _():
                arrived(rr.at[n, here], rs_sem.at[n, j])
                po[...] += rr[n, here, :].astype(jnp.float32)

            pre = po[...] * inv[here, :1] + bias[z]
            hg[z, here, :] = jnp.square(jnp.maximum(pre, 0.0)).astype(jnp.bfloat16)

            @pl.when(jnp.logical_not(last))
            def _():
                to_right(hg.at[z, here], hg.at[z, here], hg_sem.at[z, j])

            @pl.when(jnp.logical_not(first))
            def _():
                to_left(hg.at[z, here], hg.at[z, here], hg_sem.at[z, j])

        def from_left(d, _):
            s = z - d
            j = i - n - d

            @pl.when(jnp.logical_and(j >= 0, j < count))
            def _():
                here = at(j, g)
                arrived(hg.at[s, here], hg_sem.at[s, j])

                @pl.when(jnp.logical_not(last))
                def _():
                    to_right(hg.at[s, here], hg.at[s, here], hg_sem.at[s, j])

            return 0

        def from_right(d, _):
            s = z + d
            j = i - n - d

            @pl.when(jnp.logical_and(j >= 0, j < count))
            def _():
                here = at(j, g)
                arrived(hg.at[s, here], hg_sem.at[s, j])

                @pl.when(jnp.logical_not(first))
                def _():
                    to_left(hg.at[s, here], hg.at[s, here], hg_sem.at[s, j])

            return 0

        lax.fori_loop(1, z + 1, from_left, 0)
        lax.fori_loop(1, n - z, from_right, 0)

        a = i - z

        @pl.when(jnp.logical_and(a >= 0, a < count))
        def _():
            here = at(a, g)

            def segment(k, _):
                s = n - 1 - k
                part = dot(xs[here, :], uw[s])

                @pl.when(first)
                def _():
                    rr[s, here, :] = part.astype(jnp.bfloat16)

                @pl.when(jnp.logical_not(first))
                def _():
                    arrived(rr.at[s, here], rs_sem.at[s, a])
                    rr[s, here, :] = (part + rr[s, here, :].astype(jnp.float32)).astype(jnp.bfloat16)

                to_right(rr.at[s, here], rr.at[s, here], rs_sem.at[s, a])
                return 0

            lax.fori_loop(0, n - 1 - z, segment, 0)

        b = i - (n - 1 - z)

        @pl.when(jnp.logical_and(b >= 0, b < count))
        def _():
            here = at(b, g)

            def segment(s, _):
                part = dot(xs[here, :], uw[s])

                @pl.when(last)
                def _():
                    rr[s, here, :] = part.astype(jnp.bfloat16)

                @pl.when(jnp.logical_not(last))
                def _():
                    arrived(rr.at[s, here], rs_sem.at[s, b])
                    rr[s, here, :] = (part + rr[s, here, :].astype(jnp.float32)).astype(jnp.bfloat16)

                slot = jnp.where(s == z - 1, n, s)
                to_left(rr.at[s, here], rr.at[slot, here], rs_sem.at[slot, b])
                return 0

            lax.fori_loop(0, z, segment, 0)

        t = i - (2 * n - 1)
        ready = lambda t: jnp.logical_and(jnp.logical_and(t >= 0, t < count), lax.rem(t + 1, per) == 0)

        @pl.when(ready(t))
        def _():
            j = lax.div(t, per)
            here = at(j, big)
            acc[...] = dot(hg[0, here, :], dw[0])

            @pl.loop(1, n)
            def _(s):
                acc[...] += dot(hg[s, here, :], dw[s])

            ys[here, :] = acc[...].astype(jnp.bfloat16)
            yo[at(j, few), :] = acc[at(c, few), :]
            for d in range(1, m):
                peer = lax.rem(c + d, m)
                quarter = pl.ds(pl.multiple_of(j * big + peer * few, few), few)
                remote(ys.at[quarter], yr.at[c, at(j, few)], y_send.at[d], yr_sem.at[c, j], cb=peer).start()

        t1 = t - 1

        @pl.when(ready(t1))
        def _():
            j = lax.div(t1, per)
            here = at(j, few)
            branch = yo[here, :]
            for d in range(1, m):
                peer = lax.rem(c + d, m)
                arrived(yr.at[peer, here], yr_sem.at[peer, j])
                branch = branch + yr[peer, here, :].astype(jnp.float32)
            yo[here, :] = branch
            total = jnp.sum(branch * branch, axis=1, keepdims=True)
            square = jnp.concatenate([jnp.broadcast_to(total, (few, LANES))] * (LANES // few), axis=0)
            be[z, j] = square.T[:8, :]
            for d in range(1, n):
                remote(be.at[z, j], be.at[z, j], be_send.at[d], be_sem.at[z, j], ra=lax.rem(z + d, n)).start()

        t2 = t - 2

        @pl.when(ready(t2))
        def _():
            j = lax.div(t2, per)
            here = at(j, few)
            for d in range(1, n):
                s = lax.rem(z + d, n)
                arrived(be.at[s, j], be_sem.at[s, j])
            total = be[0, j]
            for s in range(1, n):
                total = total + be[s, j]
            factor = lax.rsqrt(total / width + epsilon)
            factor = jnp.broadcast_to(factor[:1, :], (LANES, LANES)).T[:few, :1]
            kept = residual_weight * xq[j].astype(jnp.float32)
            os[here, :] = (kept + yo[here, :] * factor * post_gain[...]).astype(jnp.bfloat16)
            place = pl.ds(pl.multiple_of(j * big + c * few, few), few)
            pltpu.make_async_copy(os.at[here], out.at[place], out_local).start()
            for d in range(1, m):
                peer = lax.rem(c + d, m)
                remote(os.at[here], out.at[place], o_send.at[d], out_sem.at[c], cb=peer).start()

        return 0

    lax.fori_loop(0, count + 2 * n + 1, step, 0)

    arrived(os, out_local)
    for d in range(1, m):
        arrived(os, out_sem.at[lax.rem(c + d, m)])
        arrived(os, y_send.at[d])
        arrived(os, o_send.at[d])
    for d in range(1, n):
        arrived(e.at[0], e_send.at[d])
        arrived(be.at[0], be_send.at[d])

    @pl.when(jnp.logical_not(last))
    def _():
        arrived(hg, right_sem)

    @pl.when(jnp.logical_not(first))
    def _():
        arrived(hg, left_sem)


def solution(mesh):
    n, m = mesh.shape["ra"], mesh.shape["cb"]

    def body(tokens, pre_gain, up, bias, down, post_gain):
        rows, depth = tokens.shape
        units = up.shape[1] // n
        g, big = pick(rows, n, m)
        few, blocks, count = big // m, rows // big, rows // g
        whole = pl.BlockSpec(memory_space=pl.ANY)
        inside = pl.BlockSpec(memory_space=pltpu.VMEM)
        bf16, f32, dma = jnp.bfloat16, jnp.float32, pltpu.SemaphoreType.DMA
        return pl.pallas_call(
            functools.partial(kernel, n, m, g, big),
            out_shape=jax.ShapeDtypeStruct((rows, depth), bf16),
            in_specs=[whole] * 4 + [inside] * 3,
            out_specs=whole,
            scratch_shapes=[
                pltpu.VMEM((rows, depth), bf16),
                pltpu.VMEM((n, depth, units), bf16),
                pltpu.VMEM((n, units, depth), bf16),
                pltpu.VMEM((n + 1, rows, units), bf16),
                pltpu.VMEM((n, rows, units), bf16),
                pltpu.VMEM((rows, depth), bf16),
                pltpu.VMEM((rows // m, depth), f32),
                pltpu.VMEM((m, rows // m, depth), bf16),
                pltpu.VMEM((rows // m, depth), bf16),
                pltpu.VMEM((blocks, few, depth), bf16),
                pltpu.VMEM((big, depth), f32),
                pltpu.VMEM((g, units), f32),
                pltpu.VMEM((n, 8, rows), f32),
                pltpu.VMEM((rows, LANES), f32),
                pltpu.VMEM((n, blocks, 8, LANES), f32),
                dma((n + 3,)), dma, dma, dma((n + 1, count)), dma((n, count)),
                dma((m,)), dma((m, blocks)), dma((m,)), dma((m,)), dma,
                dma((n,)), dma((n,)), dma((n,)), dma((n, blocks)),
            ],
            compiler_params=pltpu.CompilerParams(
                collective_id=0, has_side_effects=True, vmem_limit_bytes=67043328),
            name="feed_forward",
        )(tokens, tokens.reshape(blocks, m, few, depth), up, down.reshape(n, units, depth),
          pre_gain.reshape(1, depth), bias.reshape(n, 1, units), post_gain.reshape(1, depth))

    in_specs = (P("dp", "ra"), P("ra"), P("ra", "cb"), P("cb"), P("cb", "ra"), P("ra"))
    return jax.shard_map(body, mesh=mesh, in_specs=in_specs, out_specs=P("dp", "ra"), check_vma=False)
```

```python
import functools

import jax
import jax.numpy as jnp
from jax import lax
from jax.experimental import pallas as pl
from jax.experimental.pallas import tpu as pltpu
from jax.sharding import PartitionSpec as P

epsilon = 1e-06
residual_weight = 0.5
MESH = pl.DeviceIdType.MESH
LANES = 128
MOST_FLAGS = 512


def pick(rows, ra, cb):
    small = 32
    while (2 * ra + (ra + 1) // 2) * (rows // small) > MOST_FLAGS and 2 * small <= LANES:
        small *= 2
    large = small
    while large // cb < 32 and rows % (2 * large) == 0:
        large *= 2
    return small, large


def kernel(n, m, g, big, tokens, mine, up, down, pre_gain, bias, post_gain, out,
           xs, uw, dw, rr, hg, ys, yo, yr, os, xq, acc, up_sum, e, inv, be,
           load_sem, right_sem, left_sem, rs_sem, hg_sem, y_send, yr_sem, o_send, out_sem, out_local,
           e_send, e_sem, be_send, be_sem):
    rows, depth = xs.shape
    width = depth * n
    units = hg.shape[2]
    few = big // m
    count, blocks, per = rows // g, rows // big, big // g
    z, c = lax.axis_index("ra"), lax.axis_index("cb")
    first, last = z == 0, z == n - 1
    half, reach = (n + 1) // 2, n // 2
    low, high = (n - 1) // 2, n // 2
    owners = sorted({low, high})
    group = LANES // g

    def at(j, size):
        return pl.ds(pl.multiple_of(j * size, size), size)

    def remote(src, dst, send, recv, **where):
        return pltpu.make_async_remote_copy(src, dst, send, recv, device_id=where, device_id_type=MESH)

    def load_up(s):
        return pltpu.make_async_copy(up.at[:, pl.ds(pl.multiple_of(s * units, units), units)], uw.at[s], load_sem.at[s])

    head, rest = pl.ds(0, LANES), pl.ds(LANES, rows - LANES)
    load_head = pltpu.make_async_copy(tokens.at[head], ys.at[head], load_sem.at[n])
    load_rest = pltpu.make_async_copy(tokens.at[rest], ys.at[rest], load_sem.at[n + 1])
    load_mine = pltpu.make_async_copy(mine.at[:, c], xq, load_sem.at[n + 2])
    load_down = pltpu.make_async_copy(down, dw, load_sem.at[n + 3])
    load_head.start()
    for d in range(n):
        load_up(jnp.where(z <= low, n - 1 - d, d)).start()
    load_rest.start()

    barrier = pltpu.get_barrier_semaphore()
    for d in range(1, n):
        pl.semaphore_signal(barrier, inc=1, device_id={"ra": lax.rem(z + d, n)}, device_id_type=MESH)
    for d in range(1, m):
        pl.semaphore_signal(barrier, inc=1, device_id={"cb": lax.rem(c + d, m)}, device_id_type=MESH)

    def scale(b):
        part = at(b, LANES)
        raw = ys[part, :].astype(jnp.float32)
        xs[part, :] = (raw * pre_gain[...]).astype(jnp.bfloat16)
        total = jnp.sum(raw * raw, axis=1, keepdims=True)
        e[z, b] = jnp.broadcast_to(total, (LANES, LANES)).T[:8, :]

    def send_energy(b):
        for k, owner in enumerate(owners):
            @pl.when(z != owner)
            def _():
                remote(e.at[z, b], e.at[z, b], e_send.at[k], e_sem.at[z, b], ra=owner).start()

    load_head.wait()
    scale(0)
    pl.semaphore_wait(barrier, n + m - 2)
    send_energy(0)

    def dot(a, b):
        return jnp.dot(a, b, preferred_element_type=jnp.float32)

    def to_right(src, dst, flag):
        remote(src, dst, right_sem, flag, ra=jnp.minimum(z + 1, n - 1)).start()

    def to_left(src, dst, flag):
        remote(src, dst, left_sem, flag, ra=jnp.maximum(z - 1, 0)).start()

    def arrived(ref, flag):
        pltpu.make_async_copy(ref, ref, flag).wait()

    def product(s, j):
        @pl.when(j == 0)
        def _():
            load_up(s).wait()

        @pl.when(lax.rem(j, group) == 0)
        def _():
            up_sum[s] = dot(xs[at(lax.div(j, group), LANES), :], uw[s])

        return up_sum[s, at(lax.rem(j, group), g), :]

    def second(s):
        return n + jnp.where(s < half, s, s - half)

    def step(i, _):
        a = i - z

        @pl.when(jnp.logical_and(a >= 0, a < count))
        def _():
            here = at(a, g)

            def segment(k, _):
                s = n - 1 - k
                part = product(s, a)

                @pl.when(first)
                def _():
                    rr[s, here, :] = part.astype(jnp.bfloat16)

                @pl.when(jnp.logical_not(first))
                def _():
                    arrived(rr.at[s, here], rs_sem.at[s, a])
                    rr[s, here, :] = (part + rr[s, here, :].astype(jnp.float32)).astype(jnp.bfloat16)

                to_right(rr.at[s, here], rr.at[s, here], rs_sem.at[s, a])
                return 0

            lax.fori_loop(0, jnp.where(z < low, n, jnp.where(z < high, n - half, 0)), segment, 0)

        b = i - (n - 1 - z)

        @pl.when(jnp.logical_and(b >= 0, b < count))
        def _():
            here = at(b, g)

            def segment(s, _):
                part = product(s, b)

                @pl.when(last)
                def _():
                    rr[s, here, :] = part.astype(jnp.bfloat16)

                @pl.when(jnp.logical_not(last))
                def _():
                    arrived(rr.at[s, here], rs_sem.at[s, b])
                    rr[s, here, :] = (part + rr[s, here, :].astype(jnp.float32)).astype(jnp.bfloat16)

                owner = jnp.where(s < half, low, high)
                slot = jnp.where(z - 1 == owner, second(s), s)
                to_left(rr.at[s, here], rr.at[slot, here], rs_sem.at[slot, b])
                return 0

            lax.fori_loop(0, jnp.where(z > high, n, jnp.where(z > low, half, 0)), segment, 0)

        j = i - reach
        begin = jnp.where(z == low, 0, jnp.where(z == high, half, n))
        end = jnp.where(z == high, n, jnp.where(z == low, half, n))

        @pl.when(jnp.logical_and(jnp.logical_and(j >= 0, j < count), begin < end))
        def _():
            here = at(j, g)

            @pl.when(lax.rem(j, group) == 0)
            def _():
                b = lax.div(j, group)
                total = jnp.zeros((8, LANES), jnp.float32)
                for d in range(n):
                    s = lax.rem(z + d, n)
                    if d > 0:
                        arrived(e.at[s, b], e_sem.at[s, b])
                    total = total + e[s, b]
                factor = lax.rsqrt(total / width + epsilon)
                inv[...] = jnp.broadcast_to(factor[:1, :], (LANES, LANES)).T

            def segment(s, _):
                pre = product(s, j)
                if low > 0:
                    arrived(rr.at[s, here], rs_sem.at[s, j])
                    pre = pre + rr[s, here, :].astype(jnp.float32)
                elif n > 1:
                    @pl.when(jnp.logical_not(first))
                    def _():
                        arrived(rr.at[s, here], rs_sem.at[s, j])
                        spot = at(lax.rem(j, group), g)
                        up_sum[s, spot, :] += rr[s, here, :].astype(jnp.float32)

                    pre = up_sum[s, at(lax.rem(j, group), g), :]
                if high < n - 1:
                    slot = second(s)
                    arrived(rr.at[slot, here], rs_sem.at[slot, j])
                    pre = pre + rr[slot, here, :].astype(jnp.float32)
                elif n > 1:
                    @pl.when(jnp.logical_not(last))
                    def _():
                        slot = second(s)
                        arrived(rr.at[slot, here], rs_sem.at[slot, j])
                        spot = at(lax.rem(j, group), g)
                        up_sum[s, spot, :] += rr[slot, here, :].astype(jnp.float32)

                    pre = up_sum[s, at(lax.rem(j, group), g), :]
                pre = pre * inv[at(lax.rem(j, group), g), :1] + bias[s]
                hg[s, here, :] = jnp.square(jnp.maximum(pre, 0.0)).astype(jnp.bfloat16)

                @pl.when(jnp.logical_not(last))
                def _():
                    to_right(hg.at[s, here], hg.at[s, here], hg_sem.at[s, j])

                @pl.when(jnp.logical_not(first))
                def _():
                    to_left(hg.at[s, here], hg.at[s, here], hg_sem.at[s, j])

                return 0

            lax.fori_loop(begin, end, segment, 0)

        def from_left(s, _):
            j = i - reach - (z - jnp.where(s < half, low, high))

            @pl.when(jnp.logical_and(j >= 0, j < count))
            def _():
                here = at(j, g)
                arrived(hg.at[s, here], hg_sem.at[s, j])

                @pl.when(jnp.logical_not(last))
                def _():
                    to_right(hg.at[s, here], hg.at[s, here], hg_sem.at[s, j])

            return 0

        def from_right(s, _):
            j = i - reach - (jnp.where(s < half, low, high) - z)

            @pl.when(jnp.logical_and(j >= 0, j < count))
            def _():
                here = at(j, g)
                arrived(hg.at[s, here], hg_sem.at[s, j])

                @pl.when(jnp.logical_not(first))
                def _():
                    to_left(hg.at[s, here], hg.at[s, here], hg_sem.at[s, j])

            return 0

        lax.fori_loop(0, jnp.where(z > high, n, jnp.where(z > low, half, 0)), from_left, 0)
        lax.fori_loop(jnp.where(z < low, 0, jnp.where(z < high, half, n)), n, from_right, 0)

        chunk = lax.div(i * g, LANES) + 1

        @pl.when(jnp.logical_and(lax.rem(i * g, LANES) == 0, chunk < rows // LANES))
        def _():
            @pl.when(i == 0)
            def _():
                load_rest.wait()
                load_mine.start()
                load_down.start()

            scale(chunk)
            send_energy(chunk)

        t = i - 2 * reach
        ready = lambda t: jnp.logical_and(jnp.logical_and(t >= 0, t < count), lax.rem(t + 1, per) == 0)

        @pl.when(ready(t))
        def _():
            j = lax.div(t, per)
            here = at(j, big)

            @pl.when(j == 0)
            def _():
                load_down.wait()

            acc[...] = dot(hg[0, here, :], dw[0])

            @pl.loop(1, n)
            def _(s):
                acc[...] += dot(hg[s, here, :], dw[s])

            ys[here, :] = acc[...].astype(jnp.bfloat16)
            yo[at(j, few), :] = acc[at(c, few), :]
            for d in range(1, m):
                peer = lax.rem(c + d, m)
                quarter = pl.ds(pl.multiple_of(j * big + peer * few, few), few)
                remote(ys.at[quarter], yr.at[c, at(j, few)], y_send.at[d], yr_sem.at[c, j], cb=peer).start()

        t1 = t - 1

        @pl.when(ready(t1))
        def _():
            j = lax.div(t1, per)
            here = at(j, few)
            branch = yo[here, :]
            for d in range(1, m):
                peer = lax.rem(c + d, m)
                arrived(yr.at[peer, here], yr_sem.at[peer, j])
                branch = branch + yr[peer, here, :].astype(jnp.float32)
            yo[here, :] = branch
            total = jnp.sum(branch * branch, axis=1, keepdims=True)
            square = jnp.concatenate([jnp.broadcast_to(total, (few, LANES))] * (LANES // few), axis=0)
            be[z, j] = square.T[:8, :]
            for d in range(1, n):
                remote(be.at[z, j], be.at[z, j], be_send.at[d], be_sem.at[z, j], ra=lax.rem(z + d, n)).start()

        t2 = t - 2

        @pl.when(ready(t2))
        def _():
            j = lax.div(t2, per)
            here = at(j, few)

            @pl.when(j == 0)
            def _():
                load_mine.wait()

            for d in range(1, n):
                s = lax.rem(z + d, n)
                arrived(be.at[s, j], be_sem.at[s, j])
            total = be[0, j]
            for s in range(1, n):
                total = total + be[s, j]
            factor = lax.rsqrt(total / width + epsilon)
            factor = jnp.broadcast_to(factor[:1, :], (LANES, LANES)).T[:few, :1]
            kept = residual_weight * xq[j].astype(jnp.float32)
            os[here, :] = (kept + yo[here, :] * factor * post_gain[...]).astype(jnp.bfloat16)
            place = pl.ds(pl.multiple_of(j * big + c * few, few), few)
            pltpu.make_async_copy(os.at[here], out.at[place], out_local).start()
            for d in range(1, m):
                peer = lax.rem(c + d, m)
                remote(os.at[here], out.at[place], o_send.at[d], out_sem.at[c], cb=peer).start()

        return 0

    lax.fori_loop(0, count + 2 * reach + 2, step, 0)

    arrived(os, out_local)
    for d in range(1, m):
        arrived(os, out_sem.at[lax.rem(c + d, m)])
        arrived(os, y_send.at[d])
        arrived(os, o_send.at[d])
    for d in range(1, n):
        arrived(be.at[0], be_send.at[d])
    for k, owner in enumerate(owners):
        @pl.when(z != owner)
        def _():
            arrived(e.at[0], e_send.at[k])

    @pl.when(jnp.logical_not(last))
    def _():
        arrived(hg, right_sem)

    @pl.when(jnp.logical_not(first))
    def _():
        arrived(hg, left_sem)


def solution(mesh):
    n, m = mesh.shape["ra"], mesh.shape["cb"]

    def body(tokens, pre_gain, up, bias, down, post_gain):
        rows, depth = tokens.shape
        units = up.shape[1] // n
        g, big = pick(rows, n, m)
        few, blocks, count = big // m, rows // big, rows // g
        whole = pl.BlockSpec(memory_space=pl.ANY)
        inside = pl.BlockSpec(memory_space=pltpu.VMEM)
        bf16, f32, dma = jnp.bfloat16, jnp.float32, pltpu.SemaphoreType.DMA
        return pl.pallas_call(
            functools.partial(kernel, n, m, g, big),
            out_shape=jax.ShapeDtypeStruct((rows, depth), bf16),
            in_specs=[whole] * 4 + [inside] * 3,
            out_specs=whole,
            scratch_shapes=[
                pltpu.VMEM((rows, depth), bf16),
                pltpu.VMEM((n, depth, units), bf16),
                pltpu.VMEM((n, units, depth), bf16),
                pltpu.VMEM((n + (n + 1) // 2, rows, units), bf16),
                pltpu.VMEM((n, rows, units), bf16),
                pltpu.VMEM((rows, depth), bf16),
                pltpu.VMEM((rows // m, depth), f32),
                pltpu.VMEM((m, rows // m, depth), bf16),
                pltpu.VMEM((rows // m, depth), bf16),
                pltpu.VMEM((blocks, few, depth), bf16),
                pltpu.VMEM((big, depth), f32),
                pltpu.VMEM((n, LANES, units), f32),
                pltpu.VMEM((n, rows // LANES, 8, LANES), f32),
                pltpu.VMEM((LANES, LANES), f32),
                pltpu.VMEM((n, blocks, 8, LANES), f32),
                dma((n + 4,)), dma, dma, dma((n + (n + 1) // 2, count)), dma((n, count)),
                dma((m,)), dma((m, blocks)), dma((m,)), dma((m,)), dma,
                dma((n,)), dma((n, rows // LANES)), dma((n,)), dma((n, blocks)),
            ],
            compiler_params=pltpu.CompilerParams(
                collective_id=0, has_side_effects=True, vmem_limit_bytes=67043328),
            name="feed_forward",
        )(tokens, tokens.reshape(blocks, m, few, depth), up, down.reshape(n, units, depth),
          pre_gain.reshape(1, depth), bias.reshape(n, 1, units), post_gain.reshape(1, depth))

    in_specs = (P("dp", "ra"), P("ra"), P("ra", "cb"), P("cb"), P("cb", "ra"), P("ra"))
    return jax.shard_map(body, mesh=mesh, in_specs=in_specs, out_specs=P("dp", "ra"), check_vma=False)
```

```python
import functools

import jax
import jax.numpy as jnp
from jax import lax
from jax.experimental import pallas as pl
from jax.experimental.pallas import tpu as pltpu
from jax.sharding import PartitionSpec as P

epsilon = 1e-06
residual_weight = 0.5
MESH = pl.DeviceIdType.MESH
LANES = 128
MOST_FLAGS = 512


def pick(rows, ra, cb):
    small = 32
    while (2 * ra + (ra + 1) // 2) * (rows // small) > MOST_FLAGS and 2 * small <= LANES:
        small *= 2
    large = small
    while large // cb < 32 and rows % (2 * large) == 0:
        large *= 2
    tail = large
    while tail // 2 >= max(small, 16 * cb):
        tail //= 2
    return small, large, tail


def kernel(n, m, g, big, tail, tokens, up, down, pre_gain, bias, post_gain, out,
           xs, uw, dw, rr, hg, ys, yo, yr, os, xq, acc, up_sum, e, inv, be,
           load_sem, right_sem, left_sem, rs_sem, hg_sem, y_send, yr_sem, o_send, out_sem, out_local,
           e_send, e_sem, be_send, be_sem):
    rows, depth = xs.shape
    width = depth * n
    units = hg.shape[2]
    count = rows // g
    whole = rows // big - 1
    kinds = [(big, 0, whole * big // g, 0), (tail, whole * big // g, count, whole)]
    z, c = lax.axis_index("ra"), lax.axis_index("cb")
    first, last = z == 0, z == n - 1
    half, reach = (n + 1) // 2, n // 2
    low, high = (n - 1) // 2, n // 2
    owners = sorted({low, high})
    group = LANES // g

    def at(j, size):
        return pl.ds(pl.multiple_of(j * size, size), size)

    def remote(src, dst, send, recv, **where):
        return pltpu.make_async_remote_copy(src, dst, send, recv, device_id=where, device_id_type=MESH)

    def load_up(s):
        return pltpu.make_async_copy(up.at[:, pl.ds(pl.multiple_of(s * units, units), units)], uw.at[s], load_sem.at[s])

    head, rest = pl.ds(0, LANES), pl.ds(LANES, rows - LANES)
    load_head = pltpu.make_async_copy(tokens.at[head], ys.at[head], load_sem.at[n])
    load_rest = pltpu.make_async_copy(tokens.at[rest], ys.at[rest], load_sem.at[n + 1])

    def load_mine():
        for size, begin, stop, _ in kinds:
            part = size // m

            @pl.loop(0, (stop - begin) * g // size)
            def _(k):
                src = pl.ds(pl.multiple_of(begin * g + k * size + c * part, part), part)
                dst = pl.ds(pl.multiple_of(begin * g // m + k * part, part), part)
                pltpu.make_async_copy(tokens.at[src], xq.at[dst], load_sem.at[n + 2]).start()

    load_down = pltpu.make_async_copy(down, dw, load_sem.at[n + 3])
    load_head.start()
    for d in range(n):
        load_up(jnp.where(z <= low, n - 1 - d, d)).start()
    barrier = pltpu.get_barrier_semaphore()
    for d in range(1, n):
        pl.semaphore_signal(barrier, inc=1, device_id={"ra": lax.rem(z + d, n)}, device_id_type=MESH)
    for d in range(1, m):
        pl.semaphore_signal(barrier, inc=1, device_id={"cb": lax.rem(c + d, m)}, device_id_type=MESH)

    def scale(b):
        part = at(b, LANES)
        raw = ys[part, :].astype(jnp.float32)
        xs[part, :] = (raw * pre_gain[...]).astype(jnp.bfloat16)
        total = jnp.sum(raw * raw, axis=1, keepdims=True)
        e[z, b] = jnp.broadcast_to(total, (LANES, LANES)).T[:8, :]

    def send_energy(b):
        for k, owner in enumerate(owners):
            @pl.when(z != owner)
            def _():
                remote(e.at[z, b], e.at[z, b], e_send.at[k], e_sem.at[z, b], ra=owner).start()

    load_head.wait()
    scale(0)
    load_rest.start()
    pl.semaphore_wait(barrier, n + m - 2)
    send_energy(0)

    def dot(a, b):
        return jnp.dot(a, b, preferred_element_type=jnp.float32)

    def to_right(src, dst, flag):
        remote(src, dst, right_sem, flag, ra=jnp.minimum(z + 1, n - 1)).start()

    def to_left(src, dst, flag):
        remote(src, dst, left_sem, flag, ra=jnp.maximum(z - 1, 0)).start()

    def arrived(ref, flag):
        pltpu.make_async_copy(ref, ref, flag).wait()

    def product(s, j):
        @pl.when(j == 0)
        def _():
            load_up(s).wait()

        @pl.when(lax.rem(j, group) == 0)
        def _():
            up_sum[s] = dot(xs[at(lax.div(j, group), LANES), :], uw[s])

        return up_sum[s, at(lax.rem(j, group), g), :]

    def second(s):
        return n + jnp.where(s < half, s, s - half)

    def finish(t, size, begin, stop, index):
        part, steps = size // m, size // g

        def ready(t):
            inside = jnp.logical_and(t >= begin, t < stop)
            return jnp.logical_and(inside, lax.rem(t - begin + 1, steps) == 0)

        def block(t):
            k = lax.div(t - begin, steps)
            mine = pl.ds(pl.multiple_of(begin * g // m + k * part, part), part)
            return index + k, begin * g + k * size, mine

        def share(first_row, who):
            return pl.ds(pl.multiple_of(first_row + who * part, part), part)

        @pl.when(ready(t))
        def _():
            j, row, here = block(t)
            every = pl.ds(pl.multiple_of(row, size), size)

            @pl.when(j == 0)
            def _():
                load_down.wait()

            acc[:size, :] = dot(hg[0, every, :], dw[0])

            @pl.loop(1, n)
            def _(s):
                acc[:size, :] += dot(hg[s, every, :], dw[s])

            ys[every, :] = acc[:size, :].astype(jnp.bfloat16)
            yo[here, :] = acc[share(0, c), :]
            for d in range(1, m):
                peer = lax.rem(c + d, m)
                remote(ys.at[share(row, peer)], yr.at[c, here], y_send.at[d], yr_sem.at[c, j], cb=peer).start()

        @pl.when(ready(t - 1))
        def _():
            j, _, here = block(t - 1)
            branch = yo[here, :]
            for d in range(1, m):
                peer = lax.rem(c + d, m)
                arrived(yr.at[peer, here], yr_sem.at[peer, j])
                branch = branch + yr[peer, here, :].astype(jnp.float32)
            yo[here, :] = branch
            total = jnp.sum(branch * branch, axis=1, keepdims=True)
            square = jnp.concatenate([jnp.broadcast_to(total, (part, LANES))] * (LANES // part), axis=0)
            be[z, j] = square.T[:8, :]
            for d in range(1, n):
                remote(be.at[z, j], be.at[z, j], be_send.at[d], be_sem.at[z, j], ra=lax.rem(z + d, n)).start()

        @pl.when(ready(t - 2))
        def _():
            j, row, here = block(t - 2)

            @pl.when(j == 0)
            def _():
                arrived(xq, load_sem.at[n + 2])

            kept = residual_weight * xq[here, :].astype(jnp.float32)
            for d in range(1, n):
                s = lax.rem(z + d, n)
                arrived(be.at[s, j], be_sem.at[s, j])
            total = be[0, j]
            for s in range(1, n):
                total = total + be[s, j]
            factor = lax.rsqrt(total / width + epsilon)
            factor = jnp.broadcast_to(factor[:1, :], (LANES, LANES)).T[:part, :1]
            os[here, :] = (kept + yo[here, :] * factor * post_gain[...]).astype(jnp.bfloat16)
            place = share(row, c)
            pltpu.make_async_copy(os.at[here], out.at[place], out_local).start()
            for d in range(1, m):
                peer = lax.rem(c + d, m)
                remote(os.at[here], out.at[place], o_send.at[d], out_sem.at[c], cb=peer).start()

    def step(i, _):
        a = i - z

        @pl.when(jnp.logical_and(a >= 0, a < count))
        def _():
            here = at(a, g)

            def segment(k, _):
                s = n - 1 - k
                part = product(s, a)

                @pl.when(first)
                def _():
                    rr[s, here, :] = part.astype(jnp.bfloat16)

                @pl.when(jnp.logical_not(first))
                def _():
                    arrived(rr.at[s, here], rs_sem.at[s, a])
                    rr[s, here, :] = (part + rr[s, here, :].astype(jnp.float32)).astype(jnp.bfloat16)

                to_right(rr.at[s, here], rr.at[s, here], rs_sem.at[s, a])
                return 0

            lax.fori_loop(0, jnp.where(z < low, n, jnp.where(z < high, n - half, 0)), segment, 0)

        b = i - (n - 1 - z)

        @pl.when(jnp.logical_and(b >= 0, b < count))
        def _():
            here = at(b, g)

            def segment(s, _):
                part = product(s, b)

                @pl.when(last)
                def _():
                    rr[s, here, :] = part.astype(jnp.bfloat16)

                @pl.when(jnp.logical_not(last))
                def _():
                    arrived(rr.at[s, here], rs_sem.at[s, b])
                    rr[s, here, :] = (part + rr[s, here, :].astype(jnp.float32)).astype(jnp.bfloat16)

                owner = jnp.where(s < half, low, high)
                slot = jnp.where(z - 1 == owner, second(s), s)
                to_left(rr.at[s, here], rr.at[slot, here], rs_sem.at[slot, b])
                return 0

            lax.fori_loop(0, jnp.where(z > high, n, jnp.where(z > low, half, 0)), segment, 0)

        j = i - reach
        begin = jnp.where(z == low, 0, jnp.where(z == high, half, n))
        end = jnp.where(z == high, n, jnp.where(z == low, half, n))

        @pl.when(jnp.logical_and(jnp.logical_and(j >= 0, j < count), begin < end))
        def _():
            here = at(j, g)

            @pl.when(lax.rem(j, group) == 0)
            def _():
                b = lax.div(j, group)
                total = jnp.zeros((8, LANES), jnp.float32)
                for d in range(n):
                    s = lax.rem(z + d, n)
                    if d > 0:
                        arrived(e.at[s, b], e_sem.at[s, b])
                    total = total + e[s, b]
                factor = lax.rsqrt(total / width + epsilon)
                inv[...] = jnp.broadcast_to(factor[:1, :], (LANES, LANES)).T

            def segment(s, _):
                pre = product(s, j)
                if low > 0:
                    arrived(rr.at[s, here], rs_sem.at[s, j])
                    pre = pre + rr[s, here, :].astype(jnp.float32)
                elif n > 1:
                    @pl.when(jnp.logical_not(first))
                    def _():
                        arrived(rr.at[s, here], rs_sem.at[s, j])
                        spot = at(lax.rem(j, group), g)
                        up_sum[s, spot, :] += rr[s, here, :].astype(jnp.float32)

                    pre = up_sum[s, at(lax.rem(j, group), g), :]
                if high < n - 1:
                    slot = second(s)
                    arrived(rr.at[slot, here], rs_sem.at[slot, j])
                    pre = pre + rr[slot, here, :].astype(jnp.float32)
                elif n > 1:
                    @pl.when(jnp.logical_not(last))
                    def _():
                        slot = second(s)
                        arrived(rr.at[slot, here], rs_sem.at[slot, j])
                        spot = at(lax.rem(j, group), g)
                        up_sum[s, spot, :] += rr[slot, here, :].astype(jnp.float32)

                    pre = up_sum[s, at(lax.rem(j, group), g), :]
                pre = pre * inv[at(lax.rem(j, group), g), :1] + bias[s]
                hg[s, here, :] = jnp.square(jnp.maximum(pre, 0.0)).astype(jnp.bfloat16)

                @pl.when(jnp.logical_not(last))
                def _():
                    to_right(hg.at[s, here], hg.at[s, here], hg_sem.at[s, j])

                @pl.when(jnp.logical_not(first))
                def _():
                    to_left(hg.at[s, here], hg.at[s, here], hg_sem.at[s, j])

                return 0

            lax.fori_loop(begin, end, segment, 0)

        def from_left(s, _):
            j = i - reach - (z - jnp.where(s < half, low, high))

            @pl.when(jnp.logical_and(j >= 0, j < count))
            def _():
                here = at(j, g)
                arrived(hg.at[s, here], hg_sem.at[s, j])

                @pl.when(jnp.logical_not(last))
                def _():
                    to_right(hg.at[s, here], hg.at[s, here], hg_sem.at[s, j])

            return 0

        def from_right(s, _):
            j = i - reach - (jnp.where(s < half, low, high) - z)

            @pl.when(jnp.logical_and(j >= 0, j < count))
            def _():
                here = at(j, g)
                arrived(hg.at[s, here], hg_sem.at[s, j])

                @pl.when(jnp.logical_not(first))
                def _():
                    to_left(hg.at[s, here], hg.at[s, here], hg_sem.at[s, j])

            return 0

        lax.fori_loop(0, jnp.where(z > high, n, jnp.where(z > low, half, 0)), from_left, 0)
        lax.fori_loop(jnp.where(z < low, 0, jnp.where(z < high, half, n)), n, from_right, 0)

        chunk = lax.div(i * g, LANES) + 1

        @pl.when(jnp.logical_and(lax.rem(i * g, LANES) == 0, chunk < rows // LANES))
        def _():
            @pl.when(i == 0)
            def _():
                load_rest.wait()
                load_mine()
                load_down.start()

            scale(chunk)
            send_energy(chunk)

        for kind in kinds:
            finish(i - 2 * reach, *kind)

        return 0

    lax.fori_loop(0, count + 2 * reach + 2, step, 0)

    arrived(os, out_local)
    for d in range(1, m):
        arrived(os, out_sem.at[lax.rem(c + d, m)])
        arrived(os, y_send.at[d])
        arrived(os, o_send.at[d])
    for d in range(1, n):
        arrived(be.at[0], be_send.at[d])
    for k, owner in enumerate(owners):
        @pl.when(z != owner)
        def _():
            arrived(e.at[0], e_send.at[k])

    @pl.when(jnp.logical_not(last))
    def _():
        arrived(hg, right_sem)

    @pl.when(jnp.logical_not(first))
    def _():
        arrived(hg, left_sem)


def solution(mesh):
    n, m = mesh.shape["ra"], mesh.shape["cb"]

    def body(tokens, pre_gain, up, bias, down, post_gain):
        rows, depth = tokens.shape
        units = up.shape[1] // n
        g, big, tail = pick(rows, n, m)
        blocks, count = rows // big - 1 + big // tail, rows // g
        whole = pl.BlockSpec(memory_space=pl.ANY)
        inside = pl.BlockSpec(memory_space=pltpu.VMEM)
        bf16, f32, dma = jnp.bfloat16, jnp.float32, pltpu.SemaphoreType.DMA
        return pl.pallas_call(
            functools.partial(kernel, n, m, g, big, tail),
            out_shape=jax.ShapeDtypeStruct((rows, depth), bf16),
            in_specs=[whole] * 3 + [inside] * 3,
            out_specs=whole,
            scratch_shapes=[
                pltpu.VMEM((rows, depth), bf16),
                pltpu.VMEM((n, depth, units), bf16),
                pltpu.VMEM((n, units, depth), bf16),
                pltpu.VMEM((n + (n + 1) // 2, rows, units), bf16),
                pltpu.VMEM((n, rows, units), bf16),
                pltpu.VMEM((rows, depth), bf16),
                pltpu.VMEM((rows // m, depth), f32),
                pltpu.VMEM((m, rows // m, depth), bf16),
                pltpu.VMEM((rows // m, depth), bf16),
                pltpu.VMEM((rows // m, depth), bf16),
                pltpu.VMEM((big, depth), f32),
                pltpu.VMEM((n, LANES, units), f32),
                pltpu.VMEM((n, rows // LANES, 8, LANES), f32),
                pltpu.VMEM((LANES, LANES), f32),
                pltpu.VMEM((n, blocks, 8, LANES), f32),
                dma((n + 4,)), dma, dma, dma((n + (n + 1) // 2, count)), dma((n, count)),
                dma((m,)), dma((m, blocks)), dma((m,)), dma((m,)), dma,
                dma((n,)), dma((n, rows // LANES)), dma((n,)), dma((n, blocks)),
            ],
            compiler_params=pltpu.CompilerParams(
                collective_id=0, has_side_effects=True, vmem_limit_bytes=67043328),
            name="feed_forward",
        )(tokens, up, down.reshape(n, units, depth),
          pre_gain.reshape(1, depth), bias.reshape(n, 1, units), post_gain.reshape(1, depth))

    in_specs = (P("dp", "ra"), P("ra"), P("ra", "cb"), P("cb"), P("cb", "ra"), P("ra"))
    return jax.shard_map(body, mesh=mesh, in_specs=in_specs, out_specs=P("dp", "ra"), check_vma=False)
```
